256 devices in a mesh: grp: 2 (over y), sp: 32 (over z, core), tp: 4 (over x).
Axes of the slice: x: 4, y: 2, z: 16, core: 2. Of those that a mesh axis runs over, the one named last changes fastest.
The devices are a block of a 4x16x16 slice.
Arguments:
- query_nope: bfloat16 [20480, 1024], P(('grp', 'sp'), 'tp'), parts along dimension 0, may hold values from -12 to 12
- query_rope: bfloat16 [20480, 512], P(('grp', 'sp'), 'tp'), parts along dimension 0, may hold values from -48 to 48
- token_latent: bfloat16 [20480, 256], P(('grp', 'sp')), parts along dimension 0, may hold values from -6 to 6
- key_rope: bfloat16 [20480, 32], P(('grp', 'sp')), parts along dimension 0, may hold values from -48 to 48
- latent_norm_gain: float32 [256], replicated, may hold values from 0.1 to 1.9
- key_expand_weight: bfloat16 [256, 1024], replicated, may hold values from -0.375 to 0.375
- value_expand_weight: bfloat16 [256, 1024], replicated, may hold values from -0.375 to 0.375
- residual: bfloat16 [20480, 2048], P(('grp', 'sp')), parts along dimension 0, may hold values from -3 to 3
- out_weight: bfloat16 [1024, 2048], P('tp'), may hold values from -0.375 to 0.375
- ffn_gain: float32 [2048], replicated, may hold values from 0.1 to 1.9
- gate_weight: bfloat16 [2048, 5632], P('sp', 'tp'), may hold values from -0.125 to 0.125
- up_weight: bfloat16 [2048, 5632], P('sp', 'tp'), may hold values from -0.125 to 0.125
- down_weight: bfloat16 [5632, 2048], P('tp', 'sp'), may hold values from -0.078125 to 0.078125
Outputs:
- layer_output: bfloat16 [20480, 2048], P(('grp', 'sp', 'tp')), parts along dimension 0
The draws below stay inside these ranges and needn't reach their ends.
There are 2 independent parts, one for each index of `grp`. The reference program is written for one: setup_inputs(seed, part) draws one part's arguments, and reference() takes and returns one part's arrays. A program takes and returns all parts, laid end to end along the dimension named above; an argument that names none is the same for every part. Nothing has to cross between parts.
All inputs are finite; a program needn't handle non-finite values.
Results may differ from the reference program's by a relative error of at most 0.015.
Values may be sent and summed in bfloat16 or wider, within the bound.
No kernel may reach another device: no remote copies, remote signals or barrier semaphores. Data moves between devices by JAX's collectives and lax.ppermute only.
A program may use at most 128 MiB of HBM per device.

```python
import math
import jax
import jax.numpy as jnp
from jax import lax

D = 2048
HEAD_COUNT = 16
UNROTATED_SIZE = 64
ROPE = 32
VALUE_SIZE = 64
LATENT_RANK = 256
FF = 5632
GRID_W = 64
TOKEN_COUNT = 10240
N_TP = 4


def rope_pair(key):
    base = jax.random.fold_in(key, 29)
    streams = jax.random.split(base, 2)
    key_rope = jax.random.normal(streams[0], (TOKEN_COUNT, ROPE), jnp.float32)
    query_rope = 2.5 * jax.random.normal(streams[1], (TOKEN_COUNT, HEAD_COUNT * ROPE), jnp.float32)
    return (jnp.clip(key_rope, -48.0, 48.0), jnp.clip(query_rope, -48.0, 48.0))


def draw_query_rope(key, part):
    return rope_pair(key)[1].astype(jnp.bfloat16)


def draw_key_rope(key, part):
    return rope_pair(key)[0].astype(jnp.bfloat16)


def level_of(stream_key, shape, shards, low, high):
    level, own = 1.0, jax.random.fold_in(stream_key, 6)
    for axis_at, shards_of in shards:
        heights = jnp.exp(jax.random.uniform(jax.random.fold_in(own, axis_at), (shards_of,), jnp.float32, low / len(shards), high / len(shards)))
        level = level * jnp.repeat(heights, shape[axis_at] // shards_of).reshape([-1 if axis == axis_at else 1 for axis in range(len(shape))])
    return level


def gaussian(key, extent, deviation, most, cuts=(), kind=jnp.bfloat16):
    loudness = level_of(key, extent, cuts, -0.22, 0.18) if cuts else 1.0
    result = jax.random.normal(key, extent, jnp.float32) * deviation * loudness
    return jnp.minimum(jnp.maximum(result, -most), most).astype(kind)


def setup_inputs(seed: int = 0, part: int = 0) -> dict:
    key_list = jax.random.split(jax.random.key(seed), 14)
    part_keys = jax.random.split(jax.random.fold_in(key_list[13], part), 14)
    return {
        "query_nope": gaussian(part_keys[0], (TOKEN_COUNT, HEAD_COUNT * UNROTATED_SIZE), 2.5, 12.0, ((0, 32), (1, 4))),
        "query_rope": draw_query_rope(jax.random.fold_in(jax.random.fold_in(key_list[13], part), 71), part),
        "token_latent": gaussian(part_keys[2], (TOKEN_COUNT, LATENT_RANK), 1.0, 6.0, ((0, 32),)),
        "key_rope": draw_key_rope(jax.random.fold_in(jax.random.fold_in(key_list[13], part), 71), part),
        "latent_norm_gain": jnp.clip(1.0 + 0.18 * jax.random.normal(key_list[4], (LATENT_RANK,), jnp.float32), 0.1, 1.9),
        "key_expand_weight": gaussian(key_list[5], (LATENT_RANK, HEAD_COUNT * UNROTATED_SIZE), LATENT_RANK ** -0.5, 0.375),
        "value_expand_weight": gaussian(key_list[6], (LATENT_RANK, HEAD_COUNT * VALUE_SIZE), LATENT_RANK ** -0.5, 0.375),
        "residual": gaussian(part_keys[7], (TOKEN_COUNT, D), 0.5, 3.0, ((0, 32),)),
        "out_weight": gaussian(key_list[8], (HEAD_COUNT * VALUE_SIZE, D), (HEAD_COUNT * VALUE_SIZE // 4) ** -0.5, 0.375, ((0, 4),)),
        "ffn_gain": jnp.clip(1.0 + 0.18 * jax.random.normal(key_list[9], (D,), jnp.float32), 0.1, 1.9),
        "gate_weight": gaussian(key_list[10], (D, FF), D ** -0.5, 0.125, ((0, 32), (1, 4))),
        "up_weight": gaussian(key_list[11], (D, FF), D ** -0.5, 0.125, ((0, 32), (1, 4))),
        "down_weight": gaussian(key_list[12], (FF, D), FF ** -0.5, 0.078125, ((0, 4), (1, 32))),
    }


def norm_rows(values, gain):
    wide = values.astype(jnp.float32)
    return wide * lax.rsqrt(lax.optimization_barrier(jnp.mean(wide * wide, axis=-1, keepdims=True)) + 1e-06) * gain.astype(jnp.float32)

def turn_heads(vectors, positions):
    tokens, heads, width = vectors.shape
    freqs = width // 4
    grid_pos = jnp.stack([positions // GRID_W, positions % GRID_W], axis=-1).astype(jnp.float32)
    inverse = jnp.power(10000.0, -jnp.arange(freqs, dtype=jnp.float32) / freqs)
    angles = grid_pos[:, :, None] * inverse
    cosine = jnp.cos(angles)[:, None]
    sine = jnp.sin(angles)[:, None]
    viewed = vectors.reshape(tokens, heads, 2, 2, freqs)
    first = viewed[..., 0, :]
    second = viewed[..., 1, :]
    turned = jnp.stack([first * cosine - second * sine, first * sine + second * cosine], axis=-2)
    return turned.reshape(tokens, heads, width)

def reference(query_nope, query_rope, token_latent, key_rope, latent_norm_gain, key_expand_weight, value_expand_weight, residual, out_weight, ffn_gain, gate_weight, up_weight, down_weight):
    tokens = query_nope.shape[0]
    positions = jnp.arange(tokens, dtype=jnp.int32)
    query_flat = query_nope.reshape(tokens, HEAD_COUNT, UNROTATED_SIZE)
    query_turned = turn_heads(query_rope.astype(jnp.float32).reshape(tokens, HEAD_COUNT, ROPE), positions).astype(jnp.bfloat16)
    latent_normed = norm_rows(token_latent, latent_norm_gain).astype(jnp.bfloat16)
    key_turned = turn_heads(key_rope.astype(jnp.float32)[:, None, :], positions)[:, 0].astype(jnp.bfloat16)
    key_nope = jnp.dot(latent_normed, key_expand_weight, preferred_element_type=jnp.float32).astype(jnp.bfloat16)
    key_nope = key_nope.reshape(tokens, HEAD_COUNT, UNROTATED_SIZE)
    head_values = jnp.dot(latent_normed, value_expand_weight, preferred_element_type=jnp.float32).astype(jnp.bfloat16)
    head_values = head_values.reshape(tokens, HEAD_COUNT, VALUE_SIZE)
    score_scale = (UNROTATED_SIZE + ROPE) ** (-0.5)
    block_rows = math.gcd(tokens, 512)
    keys_wide = key_nope.astype(jnp.float32)
    rope_wide = key_turned.astype(jnp.float32)
    values_wide = head_values.astype(jnp.float32)

    def one_block(blocks):
        query_block, turned_block = blocks
        scores = (jnp.einsum('qhd,khd->hqk', query_block.astype(jnp.float32), keys_wide) + jnp.einsum('qhd,kd->hqk', turned_block.astype(jnp.float32), rope_wide)) * score_scale
        highest = lax.optimization_barrier(jnp.max(scores, axis=-1, keepdims=True))
        raised = jnp.exp(scores - highest)
        totals = lax.optimization_barrier(jnp.sum(raised, axis=-1))
        rounded = lax.optimization_barrier(raised.astype(jnp.bfloat16)).astype(jnp.float32)
        summed = jnp.einsum('hqk,khd->qhd', rounded, values_wide)
        return (summed / totals.T[:, :, None]).astype(jnp.bfloat16)
    attended = lax.map(one_block, (query_flat.reshape(-1, block_rows, HEAD_COUNT, UNROTATED_SIZE), query_turned.reshape(-1, block_rows, HEAD_COUNT, ROPE)))
    attended = attended.reshape(tokens, HEAD_COUNT * VALUE_SIZE)
    head_cols = HEAD_COUNT // N_TP * VALUE_SIZE
    mixed = residual.astype(jnp.float32)
    for member in range(N_TP):
        partial_out = jnp.dot(attended[:, member * head_cols:(member + 1) * head_cols], out_weight[member * head_cols:(member + 1) * head_cols], preferred_element_type=jnp.float32).astype(jnp.bfloat16)
        mixed = mixed + partial_out.astype(jnp.float32)
    normed = norm_rows(mixed, ffn_gain).astype(jnp.bfloat16)
    gate = jnp.dot(normed, gate_weight, preferred_element_type=jnp.float32)
    up_part = jnp.dot(normed, up_weight, preferred_element_type=jnp.float32)
    hidden = (jax.nn.silu(gate) * up_part).astype(jnp.bfloat16)
    hidden_cols = FF // N_TP
    layer_output = mixed
    for member in range(N_TP):
        partial_out = jnp.dot(hidden[:, member * hidden_cols:(member + 1) * hidden_cols], down_weight[member * hidden_cols:(member + 1) * hidden_cols], preferred_element_type=jnp.float32).astype(jnp.bfloat16)
        layer_output = layer_output + partial_out.astype(jnp.float32)
    return layer_output.astype(jnp.bfloat16)
```

```python
import math

import jax
import jax.numpy as jnp
import numpy as np
from jax import lax
from jax.experimental import pallas as pl
from jax.experimental.pallas import tpu as pltpu
from jax.sharding import Mesh, PartitionSpec as P


UNROTATED_SIZE = 64
ROPE = 32
VALUE_SIZE = 64
GRID_W = 64
LANES = 128
CORES = 2
BF = jnp.bfloat16
F32 = jnp.float32


NT = (((1,), (1,)), ((), ()))


def shifted(array, axis, step):
    count = lax.axis_size(axis)
    return lax.ppermute(array, axis, [(i, (i + step) % count) for i in range(count)])


def lane_index(shape):
    return lax.broadcasted_iota(jnp.int32, shape, len(shape) - 1)


def prepare_body(at, inverse, lat, gain, key, nope, rope, packed, query, cos_s, sin_s):
    rows = rope.shape[0]
    own = packed.shape[0]
    first = at[0] * rows
    lane = lane_index((rows, LANES))
    position = first + lax.broadcasted_iota(jnp.int32, (rows, LANES), 0)
    place = jnp.where((lane & 16) == 0, position >> int(math.log2(GRID_W)), position & (GRID_W - 1))
    angle = place.astype(F32) * inverse[...]
    cos_s[...] = jnp.cos(angle)
    sin_s[...] = jnp.where((lane & 8) == 0, -1.0, 1.0) * jnp.sin(angle)

    def turn(values, cosine, sine):
        wide = values.astype(F32)
        back = (lane_index(wide.shape) & 8) == 0
        other = jnp.where(back, pltpu.roll(wide, LANES - 8, 1), pltpu.roll(wide, 8, 1))
        return (wide * cosine + other * sine).astype(BF)

    width = nope.shape[1]
    query[:, :width] = nope[...]
    query[:, width:] = turn(rope[...], cos_s[...], sin_s[...])
    mine = pl.ds(pl.multiple_of(at[1] * own, 16), own)
    rank = lat.shape[1]
    wide = lat[...].astype(F32)
    scale = lax.rsqrt(jnp.mean(wide * wide, axis=-1, keepdims=True) + 1e-06)
    packed[:, :rank] = (wide * scale * gain[...]).astype(BF)
    four = jnp.concatenate([key[...]] * (LANES // ROPE), axis=1)
    packed[:, rank:] = turn(four, cos_s[mine, :], sin_s[mine, :])


def attend_body(grp, query_lat, query_rope, near, far, key_w, value_w, out, keys, values, stats):
    step = pl.program_id(0)
    pair = step % 2
    group = grp[step // 2]
    rows = query_lat.shape[1]
    half = near.shape[0]
    rank = key_w.shape[0]
    scale = (UNROTATED_SIZE + ROPE) ** (-0.5) * math.log2(math.e)

    @pl.when(step == 0)
    def _():
        keys[:half, LANES:] = near[:, rank:]
        keys[half:, LANES:] = far[:, rank:]
        values[:, LANES:] = jnp.ones((2 * half, LANES), BF)
        stats[...] = jnp.zeros(stats.shape, F32)

    both = jnp.concatenate([key_w[...], value_w[...]], axis=1)
    for at, source in ((0, near), (half, far)):
        made = jnp.dot(source[:, :rank], both, preferred_element_type=F32).astype(BF)
        keys[at : at + half, :LANES] = made[:, :LANES]
        values[at : at + half, :LANES] = made[:, LANES:]
    lane = lane_index((rows, LANES))
    zero = jnp.zeros((rows, LANES), BF)
    flat = query_lat[0]
    turned = query_rope[0]
    stacked = jnp.concatenate(
        [
            jnp.concatenate(
                [
                    jnp.where(lane // UNROTATED_SIZE == i, flat, zero),
                    jnp.where(lane // ROPE == 2 * pair + i, turned, zero),
                ],
                axis=1,
            )
            for i in range(2)
        ],
        axis=0,
    )
    scores = lax.dot_general(stacked, keys[...], NT, preferred_element_type=F32)
    highest = jnp.max(scores, axis=1, keepdims=True)
    weights = jnp.exp2((scores - highest) * scale).astype(BF)
    summed = jnp.dot(weights, values[...], preferred_element_type=F32)
    totals = summed[:, LANES:]
    mean = summed[:, :LANES] / totals
    out[2 * group + pair] = jnp.where(lane < VALUE_SIZE, mean[:rows], mean[rows:]).astype(BF)
    level = highest * scale + jnp.log2(totals)
    head = 4 * group + 2 * pair
    slot = jnp.where(lane < 48, lane % 16, -1)
    kept = jnp.where(slot == head, level[:rows], stats[...])
    stats[...] = jnp.where(slot == head + 1, level[rows:], kept)

    @pl.when(step == pl.num_programs(0) - 1)
    def _():
        whole = stats[...]
        high = whole.astype(BF)
        rest = whole - high.astype(F32)
        middle = rest.astype(BF)
        low = (rest - middle.astype(F32)).astype(BF)
        out[out.shape[0] - 1] = jnp.where(lane < 16, high, jnp.where(lane < 32, middle, low))


def merge_body(at, p0, p1, p2, p3, w0, w1, w2, w3, residual, gain, mixed, normed):
    parts = (p0, p1, p2, p3)
    rows = p0.shape[1]
    last = p0.shape[0] - 1
    levels = jnp.concatenate([p[last] for p in parts], axis=0)
    slot = lax.broadcasted_iota(jnp.int32, (LANES, LANES), 0)
    column = lane_index((LANES, LANES))
    total = residual[...].astype(F32)
    for k, weight in enumerate((w0, w1, w2, w3)):
        group = lax.rem(at[1] + (4 - k), 4)
        blocks = []
        for pair in range(2):
            head = 4 * group + 2 * pair + column // VALUE_SIZE
            spread = jnp.where((slot < 48) & (slot % 16 == head), 1.0, 0.0).astype(BF)
            wide = jnp.dot(levels, spread, preferred_element_type=F32)
            level = [wide[i * rows : (i + 1) * rows] for i in range(4)]
            top = jnp.maximum(jnp.maximum(level[0], level[1]), jnp.maximum(level[2], level[3]))
            above = jnp.zeros((rows, LANES), F32)
            below = jnp.zeros((rows, LANES), F32)
            for one, part in zip(level, parts):
                share = jnp.exp2(one - top)
                above += share * part[2 * group + pair].astype(F32)
                below += share
            blocks.append((above / below).astype(BF))
        total += jnp.dot(
            jnp.concatenate(blocks, axis=1), weight[...], preferred_element_type=F32
        )
    mixed[...] = total
    norm = lax.rsqrt(jnp.mean(total * total, axis=-1, keepdims=True) + 1e-06)
    normed[...] = (total * norm * gain[...]).astype(BF)


def feed_body(n0, n1, n2, n3, gate_w, up_w, down_w, t0, t1, t2, t3, gate, up, hidden):
    step = pl.program_id(0)
    phases = pl.num_programs(0) // 2
    width = gate_w.shape[-1]

    def flat(ref):
        return ref[...].reshape(-1, width)

    @pl.when(step < phases)
    def _():
        rows = jnp.concatenate([n0[...], n1[...], n2[...], n3[...]], axis=0)
        gate_part = jnp.dot(rows, flat(gate_w), preferred_element_type=F32)
        up_part = jnp.dot(rows, flat(up_w), preferred_element_type=F32)

        @pl.when(step == 0)
        def _():
            gate[...] = gate_part
            up[...] = up_part

        @pl.when(step > 0)
        def _():
            gate[...] += gate_part
            up[...] += up_part

    @pl.when(step == phases - 1)
    def _():
        value = gate[...]
        hidden[...] = (value / (1.0 + jnp.exp(-value)) * up[...]).astype(BF)

    @pl.when(step >= phases)
    def _():
        terms = lax.dot_general(hidden[...], flat(down_w), NT, preferred_element_type=F32)
        terms = terms.astype(BF)
        rows = t0.shape[0]
        for k, ref in enumerate((t0, t1, t2, t3)):
            ref[...] = terms[k * rows : (k + 1) * rows]


def whole(shape):
    return pl.BlockSpec(shape, lambda *_: (0,) * len(shape))


def layer(
    query_nope,
    query_rope,
    token_latent,
    key_rope,
    latent_norm_gain,
    key_expand_weight,
    value_expand_weight,
    residual,
    out_weight,
    ffn_gain,
    gate_weight,
    up_weight,
    down_weight,
):
    rows = query_nope.shape[0]
    members = lax.axis_size("tp")
    own = rows // members
    sp_count = lax.axis_size("z") * CORES
    tp_index = lax.axis_index("tp")
    sp_index = lax.axis_index("z") * CORES + lax.axis_index("core")
    at = jnp.stack([sp_index, tp_index]).astype(jnp.int32)
    rank = token_latent.shape[1]
    nope_width = query_nope.shape[1]
    rope_width = query_rope.shape[1]
    model = residual.shape[1]
    hidden_here = gate_weight.shape[1]
    share = gate_weight.shape[0]

    shards = jnp.concatenate([gate_weight, up_weight, down_weight.T], axis=0)
    gathered = lax.all_gather(shards, ("z", "core"), axis=0, tiled=True)

    freqs = ROPE // 4
    inverse = np.power(10000.0, -np.arange(freqs, dtype=np.float32) / freqs).astype(np.float32)
    inverse = jnp.asarray(np.tile(inverse, LANES // freqs)[None])
    packed, query = pl.pallas_call(
        prepare_body,
        grid_spec=pltpu.PrefetchScalarGridSpec(
            num_scalar_prefetch=1,
            grid=(1,),
            in_specs=[
                whole((1, LANES)),
                pl.BlockSpec((own, rank), lambda s, a: (a[1], 0)),
                whole((1, rank)),
                pl.BlockSpec((own, ROPE), lambda s, a: (a[1], 0)),
                whole((rows, nope_width)),
                whole((rows, rope_width)),
            ],
            out_specs=[whole((own, rank + LANES)), whole((rows, nope_width + rope_width))],
            scratch_shapes=[pltpu.VMEM((rows, LANES), F32), pltpu.VMEM((rows, LANES), F32)],
        ),
        out_shape=[
            jax.ShapeDtypeStruct((own, rank + LANES), BF),
            jax.ShapeDtypeStruct((rows, nope_width + rope_width), BF),
        ],
        name="prepare",
    )(at, inverse, token_latent, latent_norm_gain[None], key_rope, query_nope, query_rope)

    others = [shifted(query, "tp", k) for k in range(1, members)]
    queries = jnp.stack([query] + others)
    near = lax.all_gather(packed, "z", axis=0, tiled=True)
    far = shifted(near, "core", 1)
    outs = [out_weight] + [shifted(out_weight, "tp", k) for k in range(1, members)]

    group_of = lax.rem(tp_index + members - jnp.arange(members), members).astype(jnp.int32)
    keys_here = 2 * near.shape[0]
    blocks = members * nope_width // LANES
    last = blocks - 1

    def now(s):
        return jnp.minimum(s, last)

    attended = pl.pallas_call(
        attend_body,
        grid_spec=pltpu.PrefetchScalarGridSpec(
            num_scalar_prefetch=1,
            grid=(blocks,),
            in_specs=[
                pl.BlockSpec((1, rows, LANES), lambda s, g: (now(s) // 2, 0, now(s) % 2)),
                pl.BlockSpec((1, rows, LANES), lambda s, g: (now(s) // 2, 0, nope_width // LANES)),
                whole(near.shape),
                whole(near.shape),
                pl.BlockSpec((rank, LANES), lambda s, g: (0, 2 * g[now(s) // 2] + now(s) % 2)),
                pl.BlockSpec((rank, LANES), lambda s, g: (0, 2 * g[now(s) // 2] + now(s) % 2)),
            ],
            out_specs=whole((blocks + 1, rows, LANES)),
            scratch_shapes=[
                pltpu.VMEM((keys_here, 2 * LANES), BF),
                pltpu.VMEM((keys_here, 2 * LANES), BF),
                pltpu.VMEM((rows, LANES), F32),
            ],
        ),
        out_shape=jax.ShapeDtypeStruct((blocks + 1, rows, LANES), BF),
        name="attend",
    )(group_of, queries, queries, near, far, key_expand_weight, value_expand_weight)

    def block_for(step):
        where = lax.rem(tp_index + step, members) * own
        return lax.dynamic_slice_in_dim(attended, where, own, 1)

    parts = [block_for(0)] + [shifted(block_for(k), "tp", k) for k in range(1, members)]
    mixed, normed = pl.pallas_call(
        merge_body,
        grid_spec=pltpu.PrefetchScalarGridSpec(
            num_scalar_prefetch=1,
            grid=(1,),
            in_specs=[whole((blocks + 1, own, LANES))] * members
            + [whole(out_weight.shape)] * members
            + [pl.BlockSpec((own, model), lambda s, a: (a[1], 0)), whole((1, model))],
            out_specs=[whole((own, model)), whole((own, model))],
        ),
        out_shape=[
            jax.ShapeDtypeStruct((own, model), F32),
            jax.ShapeDtypeStruct((own, model), BF),
        ],
        name="merge",
    )(at, *parts, *outs, residual, ffn_gain[None])
    rows_in = [normed] + [shifted(normed, "tp", k) for k in range(1, members)]

    phases = 4
    cut = model // phases
    weights = gathered.reshape(phases, sp_count // phases, 3, share, hidden_here)

    def weight_spec(kind):
        first = kind < 2

        def index(s):
            chunk = jnp.minimum(s, phases - 1) if first else jnp.maximum(s - phases, 0)
            return (chunk, 0, kind, 0, 0)

        return pl.BlockSpec((1, sp_count // phases, 1, share, hidden_here), index)

    terms = pl.pallas_call(
        feed_body,
        grid=(2 * phases,),
        in_specs=[pl.BlockSpec((own, cut), lambda s: (0, jnp.minimum(s, phases - 1)))] * members
        + [weight_spec(kind) for kind in range(3)],
        out_specs=[pl.BlockSpec((own, cut), lambda s: (0, jnp.maximum(s - phases, 0)))] * members,
        out_shape=[jax.ShapeDtypeStruct((own, model), BF)] * members,
        scratch_shapes=[
            pltpu.VMEM((rows, hidden_here), F32),
            pltpu.VMEM((rows, hidden_here), F32),
            pltpu.VMEM((rows, hidden_here), BF),
        ],
        name="feed",
    )(*rows_in, weights, weights, weights)
    arrived = [terms[0]] + [shifted(terms[k], "tp", -k) for k in range(1, members)]
    result = mixed
    for one in arrived:
        result = result + one.astype(F32)
    return result.astype(BF)


def solution(mesh):
    groups, sp_count, members = mesh.devices.shape
    finer = Mesh(
        mesh.devices.reshape(groups, sp_count // CORES, CORES, members),
        ("grp", "z", "core", "tp"),
    )
    tokens = ("grp", "z", "core")
    return jax.shard_map(
        layer,
        mesh=finer,
        in_specs=(
            P(tokens, "tp"),
            P(tokens, "tp"),
            P(tokens, None),
            P(tokens, None),
            P(),
            P(),
            P(),
            P(tokens, None),
            P("tp", None),
            P(),
            P(("z", "core"), "tp"),
            P(("z", "core"), "tp"),
            P("tp", ("z", "core")),
        ),
        out_specs=P(tokens + ("tp",), None),
        check_vma=False,
    )
```

```python
import math

import jax
import jax.numpy as jnp
import numpy as np
from jax import lax
from jax.experimental import pallas as pl
from jax.experimental.pallas import tpu as pltpu
from jax.sharding import Mesh, PartitionSpec as P


UNROTATED_SIZE = 64
ROPE = 32
VALUE_SIZE = 64
GRID_W = 64
LANES = 128
CORES = 2
BF = jnp.bfloat16
F32 = jnp.float32


NT = (((1,), (1,)), ((), ()))


def shifted(array, axis, step):
    count = lax.axis_size(axis)
    return lax.ppermute(array, axis, [(i, (i + step) % count) for i in range(count)])


def lane_index(shape):
    return lax.broadcasted_iota(jnp.int32, shape, len(shape) - 1)


def prepare_body(at, inverse, lat, gain, key, nope, rope, packed, query, cos_s, sin_s):
    rows = rope.shape[0]
    own = packed.shape[0]
    first = at[0] * rows
    lane = lane_index((rows, LANES))
    position = first + lax.broadcasted_iota(jnp.int32, (rows, LANES), 0)
    place = jnp.where((lane & 16) == 0, position >> int(math.log2(GRID_W)), position & (GRID_W - 1))
    angle = place.astype(F32) * inverse[...]
    cos_s[...] = jnp.cos(angle)
    sin_s[...] = jnp.where((lane & 8) == 0, -1.0, 1.0) * jnp.sin(angle)

    def turn(values, cosine, sine):
        wide = values.astype(F32)
        back = (lane_index(wide.shape) & 8) == 0
        other = jnp.where(back, pltpu.roll(wide, LANES - 8, 1), pltpu.roll(wide, 8, 1))
        return (wide * cosine + other * sine).astype(BF)

    width = nope.shape[1]
    query[:, :width] = nope[...]
    query[:, width:] = turn(rope[...], cos_s[...], sin_s[...])
    mine = pl.ds(pl.multiple_of(at[1] * own, 16), own)
    rank = lat.shape[1]
    wide = lat[...].astype(F32)
    scale = lax.rsqrt(jnp.mean(wide * wide, axis=-1, keepdims=True) + 1e-06)
    packed[:, :rank] = (wide * scale * gain[...]).astype(BF)
    four = jnp.concatenate([key[...]] * (LANES // ROPE), axis=1)
    packed[:, rank:] = turn(four, cos_s[mine, :], sin_s[mine, :])


def attend_body(
    at, q0, q1, q2, q3, near, far, key_w, value_w, o0, o1, o2, o3, held, stacked, values, scores, highest, stats
):
    step = pl.program_id(0)
    last = pl.num_programs(0) - 1
    turn = step // 2
    pair = step % 2
    group = lax.rem(at[1] + 4 - turn, 4)
    rows = q0.shape[0]
    own = o0.shape[1]
    half = near.shape[0]
    rank = key_w.shape[0]
    scale = (UNROTATED_SIZE + ROPE) ** (-0.5) * math.log2(math.e)
    tile = 256
    wide = 2 * tile
    chunks = 2 * half // wide
    lane = lane_index((rows, LANES))

    @pl.when(step == 0)
    def _():
        values[:, LANES:] = jnp.ones((2 * half, LANES), BF)
        stats[...] = jnp.zeros(stats.shape, F32)

    zero = jnp.zeros((rows, LANES), BF)
    for k, query in enumerate((q0, q1, q2, q3)):
        for p in range(2):

            @pl.when(step == 2 * k + p)
            def _():
                flat = query[:, p * LANES : (p + 1) * LANES]
                turned = query[:, 2 * LANES :]
                for i in range(2):
                    mine = slice(i * rows, (i + 1) * rows)
                    stacked[mine, :LANES] = jnp.where(lane // UNROTATED_SIZE == i, flat, zero)
                    stacked[mine, LANES:] = jnp.where(lane // ROPE == 2 * p + i, turned, zero)

    both = jnp.concatenate([key_w[...], value_w[...]], axis=1)
    asked = stacked[...]
    for c in range(chunks):
        top = None
        for u in (c, c + chunks):
            source, from_row = (near, u * tile) if u < chunks else (far, u * tile - half)
            made = jnp.dot(
                source[from_row : from_row + tile, :rank], both, preferred_element_type=F32
            ).astype(BF)
            values[u * tile : (u + 1) * tile, :LANES] = made[:, LANES:]
            keys = jnp.concatenate([made[:, :LANES], source[from_row : from_row + tile, rank:]], axis=1)
            part = lax.dot_general(asked, keys, NT, preferred_element_type=F32)
            scores[:, u * tile : (u + 1) * tile] = part
            level = jnp.maximum(part[:, :LANES], part[:, LANES:])
            top = level if top is None else jnp.maximum(top, level)
        highest[...] = top if c == 0 else jnp.maximum(highest[...], top)

    @pl.when(step <= last)
    def _():
        peak = jnp.broadcast_to(jnp.max(highest[...], axis=1, keepdims=True), (2 * rows, LANES))
        many = jnp.concatenate([peak] * (wide // LANES), axis=1)
        summed = None
        for c in range(chunks):
            spot = slice(c * wide, (c + 1) * wide)
            weights = jnp.exp2((scores[:, spot] - many) * scale).astype(BF)
            more = jnp.dot(weights, values[spot, :], preferred_element_type=F32)
            summed = more if c == 0 else summed + more
        totals = summed[:, LANES:]
        mean = summed[:, :LANES] / totals
        held[2 * group + pair] = jnp.where(lane < VALUE_SIZE, mean[:rows], mean[rows:]).astype(BF)
        level = peak * scale + jnp.log2(totals)
        head = 4 * group + 2 * pair
        place = jnp.where(lane < 48, lane % 16, -1)
        kept = jnp.where(place == head, level[:rows], stats[...])
        stats[...] = jnp.where(place == head + 1, level[rows:], kept)

    @pl.when(step == last)
    def _():
        every = stats[...]
        high = every.astype(BF)
        rest = every - high.astype(F32)
        middle = rest.astype(BF)
        low = (rest - middle.astype(F32)).astype(BF)
        held[held.shape[0] - 1] = jnp.where(lane < 16, high, jnp.where(lane < 32, middle, low))
        for k, ref in enumerate((o0, o1, o2, o3)):
            start = pl.multiple_of(lax.rem(at[1] + k, 4) * own, 16)
            ref[...] = held[:, pl.ds(start, own), :]


def merge_body(at, p0, p1, p2, p3, w0, w1, w2, w3, residual, gain, mixed, normed_a, normed_b):
    parts = (p0, p1, p2, p3)
    rows = p0.shape[1]
    last = p0.shape[0] - 1
    levels = jnp.concatenate([p[last] for p in parts], axis=0)
    slot = lax.broadcasted_iota(jnp.int32, (LANES, LANES), 0)
    column = lane_index((LANES, LANES))
    total = residual[...].astype(F32)
    for k, weight in enumerate((w0, w1, w2, w3)):
        group = lax.rem(at[1] + (4 - k), 4)
        blocks = []
        for pair in range(2):
            head = 4 * group + 2 * pair + column // VALUE_SIZE
            spread = jnp.where((slot < 48) & (slot % 16 == head), 1.0, 0.0).astype(BF)
            wide = jnp.dot(levels, spread, preferred_element_type=F32)
            level = [wide[i * rows : (i + 1) * rows] for i in range(4)]
            top = jnp.maximum(jnp.maximum(level[0], level[1]), jnp.maximum(level[2], level[3]))
            above = jnp.zeros((rows, LANES), F32)
            below = jnp.zeros((rows, LANES), F32)
            for one, part in zip(level, parts):
                share = jnp.exp2(one - top)
                above += share * part[2 * group + pair].astype(F32)
                below += share
            blocks.append((above / below).astype(BF))
        total += jnp.dot(
            jnp.concatenate(blocks, axis=1), weight[...], preferred_element_type=F32
        )
    mixed[...] = total
    norm = lax.rsqrt(jnp.mean(total * total, axis=-1, keepdims=True) + 1e-06)
    normed = (total * norm * gain[...]).astype(BF)
    half = normed_a.shape[1]
    normed_a[...] = normed[:, :half]
    normed_b[...] = normed[:, half:]


def feed_body(*refs):
    pieces, weights, refs = refs[:8], refs[8], refs[9:]
    ends, (rows_in, kept, gate, up, hidden, sems) = refs[:8], refs[8:]
    phases, per, _, share, width = kept.shape
    own, half = pieces[0].shape
    cut = rows_in.shape[2]

    def copy_of(chunk, member, first, count, sem):
        spot = (chunk, member, pl.ds(first, count))
        return pltpu.make_async_copy(weights.at[spot], kept.at[spot], sem)

    def early(chunk, member):
        return copy_of(chunk, member, 0, 2, sems.at[0, chunk, member])

    def late(chunk, member):
        return copy_of(chunk, member, 2, 1, sems.at[1, chunk, member])

    for make in (early, late):
        for chunk in range(phases):
            for member in range(per):
                make(chunk, member).start()
    for chunk in range(phases):
        side, at = divmod(chunk * cut, half)
        for k in range(4):
            rows_in[chunk, k * own : (k + 1) * own] = pieces[2 * k + side][:, at : at + cut]
    gate[...] = jnp.zeros(gate.shape, F32)
    up[...] = jnp.zeros(up.shape, F32)

    def widen(chunk, carry):
        for member in range(per):
            early(chunk, member).wait()
        rows = rows_in[chunk]
        gate[...] += jnp.dot(
            rows, kept[chunk, :, 0].reshape(per * share, width), preferred_element_type=F32
        )
        up[...] += jnp.dot(
            rows, kept[chunk, :, 1].reshape(per * share, width), preferred_element_type=F32
        )
        return carry

    lax.fori_loop(0, phases, widen, 0)
    value = gate[...]
    hidden[...] = (value / (1.0 + jnp.exp(-value)) * up[...]).astype(BF)
    for chunk in range(phases):
        for member in range(per):
            late(chunk, member).wait()
        terms = lax.dot_general(
            hidden[...],
            kept[chunk, :, 2].reshape(per * share, width),
            NT,
            preferred_element_type=F32,
        ).astype(BF)
        side, at = divmod(chunk * cut, half)
        for k in range(4):
            ends[4 * side + k][:, at : at + cut] = terms[k * own : (k + 1) * own]


def room(mib):
    return pltpu.CompilerParams(vmem_limit_bytes=mib * 1024 * 1024)


def whole(shape):
    return pl.BlockSpec(shape, lambda *_: (0,) * len(shape))


def layer(
    query_nope,
    query_rope,
    token_latent,
    key_rope,
    latent_norm_gain,
    key_expand_weight,
    value_expand_weight,
    residual,
    out_weight,
    ffn_gain,
    gate_weight,
    up_weight,
    down_weight,
):
    rows = query_nope.shape[0]
    members = lax.axis_size("tp")
    own = rows // members
    sp_count = lax.axis_size("z") * CORES
    tp_index = lax.axis_index("tp")
    sp_index = lax.axis_index("z") * CORES + lax.axis_index("core")
    at = jnp.stack([sp_index, tp_index]).astype(jnp.int32)
    rank = token_latent.shape[1]
    nope_width = query_nope.shape[1]
    rope_width = query_rope.shape[1]
    model = residual.shape[1]
    hidden_here = gate_weight.shape[1]
    share = gate_weight.shape[0]

    shards = jnp.concatenate([gate_weight, up_weight, down_weight.T], axis=0)
    gathered = lax.all_gather(shards, ("z", "core"), axis=0, tiled=True)

    freqs = ROPE // 4
    inverse = np.power(10000.0, -np.arange(freqs, dtype=np.float32) / freqs).astype(np.float32)
    inverse = jnp.asarray(np.tile(inverse, LANES // freqs)[None])
    packed, query = pl.pallas_call(
        prepare_body,
        grid_spec=pltpu.PrefetchScalarGridSpec(
            num_scalar_prefetch=1,
            grid=(1,),
            in_specs=[
                whole((1, LANES)),
                pl.BlockSpec((own, rank), lambda s, a: (a[1], 0)),
                whole((1, rank)),
                pl.BlockSpec((own, ROPE), lambda s, a: (a[1], 0)),
                whole((rows, nope_width)),
                whole((rows, rope_width)),
            ],
            out_specs=[whole((own, rank + LANES)), whole((rows, nope_width + rope_width))],
            scratch_shapes=[pltpu.VMEM((rows, LANES), F32), pltpu.VMEM((rows, LANES), F32)],
        ),
        out_shape=[
            jax.ShapeDtypeStruct((own, rank + LANES), BF),
            jax.ShapeDtypeStruct((rows, nope_width + rope_width), BF),
        ],
        compiler_params=room(8),
        name="prepare",
    )(at, inverse, token_latent, latent_norm_gain[None], key_rope, query_nope, query_rope)

    others = [shifted(query, "tp", k) for k in range(1, members)]
    near = lax.all_gather(packed, "z", axis=0, tiled=True)
    far = shifted(near, "core", 1)
    outs = [out_weight] + [shifted(out_weight, "tp", k) for k in range(1, members)]

    keys_here = 2 * near.shape[0]
    blocks = members * nope_width // LANES
    part = (blocks + 1, own, LANES)

    def group_at(s, a):
        return lax.rem(a[1] + members - s // 2, members)

    attended = pl.pallas_call(
        attend_body,
        grid_spec=pltpu.PrefetchScalarGridSpec(
            num_scalar_prefetch=1,
            grid=(blocks,),
            in_specs=[whole(query.shape)] * members
            + [whole(near.shape)] * 2
            + [pl.BlockSpec((rank, LANES), lambda s, a: (0, 2 * group_at(s, a) + s % 2))] * 2,
            out_specs=[whole(part)] * members,
            scratch_shapes=[
                pltpu.VMEM((blocks + 1, rows, LANES), BF),
                pltpu.VMEM((2 * rows, 2 * LANES), BF),
                pltpu.VMEM((keys_here, 2 * LANES), BF),
                pltpu.VMEM((2 * rows, keys_here), F32),
                pltpu.VMEM((2 * rows, LANES), F32),
                pltpu.VMEM((rows, LANES), F32),
            ],
        ),
        out_shape=[jax.ShapeDtypeStruct(part, BF)] * members,
        compiler_params=room(32),
        name="attend",
    )(at, query, *others, near, far, key_expand_weight, value_expand_weight)
    parts = [attended[0]] + [shifted(attended[k], "tp", k) for k in range(1, members)]
    half = model // 2
    mixed, own_a, own_b = pl.pallas_call(
        merge_body,
        grid_spec=pltpu.PrefetchScalarGridSpec(
            num_scalar_prefetch=1,
            grid=(1,),
            in_specs=[whole(part)] * members
            + [whole(out_weight.shape)] * members
            + [pl.BlockSpec((own, model), lambda s, a: (a[1], 0)), whole((1, model))],
            out_specs=[whole((own, model)), whole((own, half)), whole((own, half))],
        ),
        out_shape=[
            jax.ShapeDtypeStruct((own, model), F32),
            jax.ShapeDtypeStruct((own, half), BF),
            jax.ShapeDtypeStruct((own, half), BF),
        ],
        compiler_params=room(20),
        name="merge",
    )(at, *parts, *outs, residual, ffn_gain[None])
    below_a = shifted(own_a, "tp", 1)
    above_b = shifted(own_b, "tp", -1)
    below_b = shifted(own_b, "tp", 1)
    above_a = shifted(own_a, "tp", -1)
    across_a = shifted(below_a, "tp", 1)
    across_b = shifted(above_b, "tp", -1)

    phases = 4
    cut = model // phases
    weights = gathered.reshape(phases, sp_count // phases, 3, share, hidden_here)
    terms = pl.pallas_call(
        feed_body,
        in_specs=[pl.BlockSpec(memory_space=pltpu.VMEM)] * 8 + [pl.BlockSpec(memory_space=pl.ANY)],
        out_specs=[pl.BlockSpec(memory_space=pltpu.VMEM)] * 8,
        out_shape=[jax.ShapeDtypeStruct((own, half), BF)] * 8,
        scratch_shapes=[
            pltpu.VMEM((phases, rows, cut), BF),
            pltpu.VMEM(weights.shape, BF),
            pltpu.VMEM((rows, hidden_here), F32),
            pltpu.VMEM((rows, hidden_here), F32),
            pltpu.VMEM((rows, hidden_here), BF),
            pltpu.SemaphoreType.DMA((2, phases, sp_count // phases)),
        ],
        compiler_params=room(40),
        name="feed",
    )(own_a, own_b, below_a, below_b, across_a, across_b, above_a, above_b, weights)
    mine_a, down_a, far_a, up_a, mine_b, down_b, far_b, up_b = terms
    far_a = shifted(far_a, "tp", -1)
    far_b = shifted(far_b, "tp", 1)
    from_above_b = shifted(down_b, "tp", -1)
    from_below_a = shifted(up_a, "tp", 1)
    from_above_a = shifted((down_a.astype(F32) + far_a.astype(F32)).astype(BF), "tp", -1)
    from_below_b = shifted((up_b.astype(F32) + far_b.astype(F32)).astype(BF), "tp", 1)

    def added(base, *more):
        for one in more:
            base = base + one.astype(F32)
        return base.astype(BF)

    return jnp.concatenate(
        [
            added(mixed[:, :half], mine_a, from_above_a, from_below_a),
            added(mixed[:, half:], mine_b, from_above_b, from_below_b),
        ],
        axis=1,
    )


def solution(mesh):
    groups, sp_count, members = mesh.devices.shape
    finer = Mesh(
        mesh.devices.reshape(groups, sp_count // CORES, CORES, members),
        ("grp", "z", "core", "tp"),
    )
    tokens = ("grp", "z", "core")
    return jax.shard_map(
        layer,
        mesh=finer,
        in_specs=(
            P(tokens, "tp"),
            P(tokens, "tp"),
            P(tokens, None),
            P(tokens, None),
            P(),
            P(),
            P(),
            P(tokens, None),
            P("tp", None),
            P(),
            P(("z", "core"), "tp"),
            P(("z", "core"), "tp"),
            P("tp", ("z", "core")),
        ),
        out_specs=P(tokens + ("tp",), None),
        check_vma=False,
    )
```

```python
import math

import jax
import jax.numpy as jnp
import numpy as np
from jax import lax
from jax.experimental import pallas as pl
from jax.experimental.pallas import tpu as pltpu
from jax.sharding import Mesh, PartitionSpec as P


UNROTATED_SIZE = 64
ROPE = 32
VALUE_SIZE = 64
GRID_W = 64
LANES = 128
CORES = 2
PART = 16
BF = jnp.bfloat16
F32 = jnp.float32


NT = (((1,), (1,)), ((), ()))


def shifted(array, axis, step):
    count = lax.axis_size(axis)
    return lax.ppermute(array, axis, [(i, (i + step) % count) for i in range(count)])


def lane_index(shape):
    return lax.broadcasted_iota(jnp.int32, shape, len(shape) - 1)


def close_body(mixed, a0, a1, a2, b0, b1, b2, out):
    half = a0.shape[1]
    for at, parts in ((0, (a0, a1, a2)), (half, (b0, b1, b2))):
        total = mixed[:, at : at + half]
        for part in parts:
            total += part[...].astype(F32)
        out[:, at : at + half] = total.astype(BF)


def prepare_body(at, inverse, lat, gain, key, nope, rope, packed, query, cos_s, sin_s):
    rows = rope.shape[0]
    own = lat.shape[0]
    start = at[0] * rows
    lane = lane_index((rows, LANES))
    position = start + lax.broadcasted_iota(jnp.int32, (rows, LANES), 0)
    place = jnp.where((lane & 16) == 0, position >> int(math.log2(GRID_W)), position & (GRID_W - 1))
    angle = place.astype(F32) * inverse[...]
    cos_s[...] = jnp.cos(angle)
    sin_s[...] = jnp.where((lane & 8) == 0, -1.0, 1.0) * jnp.sin(angle)

    def turn(values, cosine, sine):
        wide = values.astype(F32)
        back = (lane_index(wide.shape) & 8) == 0
        other = jnp.where(back, pltpu.roll(wide, LANES - 8, 1), pltpu.roll(wide, 8, 1))
        return (wide * cosine + other * sine).astype(BF)

    width = nope.shape[1]
    query[:, :width] = nope[...]
    query[:, width:] = turn(rope[...], cos_s[...], sin_s[...])
    mine = pl.ds(pl.multiple_of(at[1] * own, 16), own)
    rank = lat.shape[1]
    wide = lat[...].astype(F32)
    scale = lax.rsqrt(jnp.mean(wide * wide, axis=-1, keepdims=True) + 1e-06)
    normed = (wide * scale * gain[...]).astype(BF)
    for j in range(rank // LANES):
        packed[j * own : (j + 1) * own] = normed[:, j * LANES : (j + 1) * LANES]
    four = jnp.concatenate([key[...]] * (LANES // ROPE), axis=1)
    turned = turn(four, cos_s[mine, :], sin_s[mine, :])
    place = lane_index((PART, LANES)) // ROPE
    first = turned[:PART]
    for j in range(1, LANES // ROPE):
        first = jnp.where(place == j, turned[j * PART : (j + 1) * PART], first)
    at_row = rank // LANES * own
    packed[at_row : at_row + PART] = first
    packed[at_row + PART : at_row + 2 * PART] = turned[LANES // ROPE * PART :]


def attend_body(
    at, q0, q1, q2, q3, near, far, key_w, value_w, o0, o1, o2, o3, held, stacked, latents, ropes, values, scores, highest, stats
):
    step = pl.program_id(0)
    last = pl.num_programs(0) - 1
    turn = step // 2
    pair = step % 2
    group = lax.rem(at[1] + 4 - turn, 4)
    rows = q0.shape[0]
    own = o0.shape[1]
    places = near.shape[0]
    half = places * own
    rank = key_w.shape[0]
    scale = (UNROTATED_SIZE + ROPE) ** (-0.5) * math.log2(math.e)
    tile = 256
    wide = 2 * tile
    chunks = 2 * half // wide
    lane = lane_index((rows, LANES))

    @pl.when(step == 0)
    def _():
        values[:, LANES:] = jnp.ones((2 * half, LANES), BF)
        stats[...] = jnp.zeros(stats.shape, F32)
        splits = LANES // ROPE
        head_row = rank // LANES * own
        spot = lane_index((places * PART, LANES)) // ROPE
        for h, source in enumerate((near, far)):
            mixed = source[:, head_row : head_row + PART].reshape(places * PART, LANES).astype(F32)
            rolled = [mixed] + [pltpu.roll(mixed, ROPE * k, 1) for k in range(1, splits)]
            for j in range(splits):
                full = rolled[(splits - j) % splits]
                for lanes_at in range(1, splits):
                    full = jnp.where(spot == lanes_at, rolled[(lanes_at - j) % splits], full)
                full = full.astype(BF)
                for z in range(places):
                    row = h * half + z * own + j * PART
                    ropes[row : row + PART] = full[z * PART : (z + 1) * PART]
            for z in range(places):
                row = h * half + z * own
                ropes[row + splits * PART : row + own] = source[z, head_row + PART :]
                for j in range(rank // LANES):
                    latents[row : row + own, j * LANES : (j + 1) * LANES] = source[
                        z, j * own : (j + 1) * own
                    ]

    zero = jnp.zeros((rows, LANES), BF)
    for k, query in enumerate((q0, q1, q2, q3)):
        for p in range(2):

            @pl.when(step == 2 * k + p)
            def _():
                flat = query[:, p * LANES : (p + 1) * LANES]
                turned = query[:, 2 * LANES :]
                for i in range(2):
                    mine = slice(i * rows, (i + 1) * rows)
                    stacked[mine, :LANES] = jnp.where(lane // UNROTATED_SIZE == i, flat, zero)
                    stacked[mine, LANES:] = jnp.where(lane // ROPE == 2 * p + i, turned, zero)

    both = jnp.concatenate([key_w[...], value_w[...]], axis=1)
    asked = stacked[...]
    for c in range(chunks):
        top = None
        for u in (c, c + chunks):
            spot = slice(u * tile, (u + 1) * tile)
            made = jnp.dot(latents[spot], both, preferred_element_type=F32).astype(BF)
            values[spot, :LANES] = made[:, LANES:]
            keys = jnp.concatenate([made[:, :LANES], ropes[spot]], axis=1)
            part = lax.dot_general(asked, keys, NT, preferred_element_type=F32)
            scores[:, spot] = part
            level = jnp.maximum(part[:, :LANES], part[:, LANES:])
            top = level if top is None else jnp.maximum(top, level)
        highest[...] = top if c == 0 else jnp.maximum(highest[...], top)

    @pl.when(step <= last)
    def _():
        peak = jnp.broadcast_to(jnp.max(highest[...], axis=1, keepdims=True), (2 * rows, LANES))
        many = jnp.concatenate([peak] * (wide // LANES), axis=1)
        summed = None
        for c in range(chunks):
            spot = slice(c * wide, (c + 1) * wide)
            weights = jnp.exp2((scores[:, spot] - many) * scale).astype(BF)
            more = jnp.dot(weights, values[spot, :], preferred_element_type=F32)
            summed = more if c == 0 else summed + more
        totals = summed[:, LANES:]
        mean = summed[:, :LANES] / totals
        held[2 * group + pair] = jnp.where(lane < VALUE_SIZE, mean[:rows], mean[rows:]).astype(BF)
        level = peak * scale + jnp.log2(totals)
        head = 4 * group + 2 * pair
        place = jnp.where(lane < 48, lane % 16, -1)
        kept = jnp.where(place == head, level[:rows], stats[...])
        stats[...] = jnp.where(place == head + 1, level[rows:], kept)

    @pl.when(step == last)
    def _():
        every = stats[...]
        high = every.astype(BF)
        rest = every - high.astype(F32)
        middle = rest.astype(BF)
        low = (rest - middle.astype(F32)).astype(BF)
        held[held.shape[0] - 1] = jnp.where(lane < 16, high, jnp.where(lane < 32, middle, low))
        for k, ref in enumerate((o0, o1, o2, o3)):
            start = pl.multiple_of(lax.rem(at[1] + k, 4) * own, 16)
            ref[...] = held[:, pl.ds(start, own), :]


def merge_body(at, p0, p1, p2, p3, w0, w1, w2, w3, residual, gain, mixed, normed_a, normed_b):
    parts = (p0, p1, p2, p3)
    rows = p0.shape[1]
    last = p0.shape[0] - 1
    levels = jnp.concatenate([p[last] for p in parts], axis=0)
    slot = lax.broadcasted_iota(jnp.int32, (LANES, LANES), 0)
    column = lane_index((LANES, LANES))
    total = residual[...].astype(F32)
    for k, weight in enumerate((w0, w1, w2, w3)):
        group = lax.rem(at[1] + (4 - k), 4)
        blocks = []
        for pair in range(2):
            head = 4 * group + 2 * pair + column // VALUE_SIZE
            spread = jnp.where((slot < 48) & (slot % 16 == head), 1.0, 0.0).astype(BF)
            wide = jnp.dot(levels, spread, preferred_element_type=F32)
            level = [wide[i * rows : (i + 1) * rows] for i in range(4)]
            top = jnp.maximum(jnp.maximum(level[0], level[1]), jnp.maximum(level[2], level[3]))
            above = jnp.zeros((rows, LANES), F32)
            below = jnp.zeros((rows, LANES), F32)
            for one, part in zip(level, parts):
                share = jnp.exp2(one - top)
                above += share * part[2 * group + pair].astype(F32)
                below += share
            blocks.append((above / below).astype(BF))
        total += jnp.dot(
            jnp.concatenate(blocks, axis=1), weight[...], preferred_element_type=F32
        )
    mixed[...] = total
    norm = lax.rsqrt(jnp.mean(total * total, axis=-1, keepdims=True) + 1e-06)
    normed = (total * norm * gain[...]).astype(BF)
    half = normed_a.shape[1]
    normed_a[...] = normed[:, :half]
    normed_b[...] = normed[:, half:]


def feed_body(*refs):
    pieces, weights, refs = refs[:8], refs[8], refs[9:]
    ends, (rows_in, kept, gate, up, hidden, sems) = refs[:8], refs[8:]
    phases, per, _, share, width = kept.shape
    own, half = pieces[0].shape
    cut = rows_in.shape[2]

    def copy_of(chunk, member, first, count, sem):
        spot = (chunk, member, pl.ds(first, count))
        return pltpu.make_async_copy(weights.at[spot], kept.at[spot], sem)

    def early(chunk, member):
        return copy_of(chunk, member, 0, 2, sems.at[0, chunk, member])

    def late(chunk, member):
        return copy_of(chunk, member, 2, 1, sems.at[1, chunk, member])

    def begin(make, chunk):
        for member in range(per):
            make(chunk, member).start()

    begin(early, 0)
    begin(early, 1)
    for chunk in range(phases):
        side, at = divmod(chunk * cut, half)
        for k in range(4):
            rows_in[chunk, k * own : (k + 1) * own] = pieces[2 * k + side][:, at : at + cut]
    gate[...] = jnp.zeros(gate.shape, F32)
    up[...] = jnp.zeros(up.shape, F32)

    def widen(chunk, carry):
        for member in range(per):
            early(chunk, member).wait()

        @pl.when(chunk + 2 < phases)
        def _():
            begin(early, chunk + 2)

        @pl.when(chunk + 2 >= phases)
        def _():
            begin(late, chunk + 2 - phases)

        rows = rows_in[chunk]
        gate[...] += jnp.dot(
            rows, kept[chunk, :, 0].reshape(per * share, width), preferred_element_type=F32
        )
        up[...] += jnp.dot(
            rows, kept[chunk, :, 1].reshape(per * share, width), preferred_element_type=F32
        )
        return carry

    lax.fori_loop(0, phases, widen, 0)
    for chunk in range(2, phases):
        begin(late, chunk)
    value = gate[...]
    hidden[...] = (value / (1.0 + jnp.exp(-value)) * up[...]).astype(BF)
    for chunk in range(phases):
        for member in range(per):
            late(chunk, member).wait()
        terms = lax.dot_general(
            hidden[...],
            kept[chunk, :, 2].reshape(per * share, width),
            NT,
            preferred_element_type=F32,
        ).astype(BF)
        side, at = divmod(chunk * cut, half)
        for k in range(4):
            ends[4 * side + k][:, at : at + cut] = terms[k * own : (k + 1) * own]


def room(mib):
    return pltpu.CompilerParams(vmem_limit_bytes=mib * 1024 * 1024)


def whole(shape):
    return pl.BlockSpec(shape, lambda *_: (0,) * len(shape))


def layer(
    query_nope,
    query_rope,
    token_latent,
    key_rope,
    latent_norm_gain,
    key_expand_weight,
    value_expand_weight,
    residual,
    out_weight,
    ffn_gain,
    gate_weight,
    up_weight,
    down_weight,
):
    rows = query_nope.shape[0]
    members = lax.axis_size("tp")
    own = rows // members
    sp_count = lax.axis_size("z") * CORES
    tp_index = lax.axis_index("tp")
    sp_index = lax.axis_index("z") * CORES + lax.axis_index("core")
    at = jnp.stack([sp_index, tp_index]).astype(jnp.int32)
    rank = token_latent.shape[1]
    nope_width = query_nope.shape[1]
    rope_width = query_rope.shape[1]
    model = residual.shape[1]
    hidden_here = gate_weight.shape[1]
    share = gate_weight.shape[0]

    shards = jnp.concatenate([gate_weight, up_weight, down_weight.T], axis=0)
    gathered = lax.all_gather(shards, ("z", "core"), axis=0, tiled=True)

    freqs = ROPE // 4
    inverse = np.power(10000.0, -np.arange(freqs, dtype=np.float32) / freqs).astype(np.float32)
    inverse = jnp.asarray(np.tile(inverse, LANES // freqs)[None])
    packed_shape = (rank // LANES * own + 2 * PART, LANES)
    packed, query = pl.pallas_call(
        prepare_body,
        grid_spec=pltpu.PrefetchScalarGridSpec(
            num_scalar_prefetch=1,
            grid=(1,),
            in_specs=[
                whole((1, LANES)),
                pl.BlockSpec((own, rank), lambda s, a: (a[1], 0)),
                whole((1, rank)),
                pl.BlockSpec((own, ROPE), lambda s, a: (a[1], 0)),
                whole((rows, nope_width)),
                whole((rows, rope_width)),
            ],
            out_specs=[whole(packed_shape), whole((rows, nope_width + rope_width))],
            scratch_shapes=[pltpu.VMEM((rows, LANES), F32), pltpu.VMEM((rows, LANES), F32)],
        ),
        out_shape=[
            jax.ShapeDtypeStruct(packed_shape, BF),
            jax.ShapeDtypeStruct((rows, nope_width + rope_width), BF),
        ],
        compiler_params=room(8),
        name="prepare",
    )(at, inverse, token_latent, latent_norm_gain[None], key_rope, query_nope, query_rope)

    others = [shifted(query, "tp", k) for k in range(1, members)]
    near = lax.all_gather(packed, "z", axis=0, tiled=True)
    near = near.reshape(-1, *packed_shape)
    far = shifted(near, "core", 1)
    outs = [out_weight] + [shifted(out_weight, "tp", k) for k in range(1, members)]

    keys_here = 2 * near.shape[0] * own
    blocks = members * nope_width // LANES
    part = (blocks + 1, own, LANES)

    def group_at(s, a):
        return lax.rem(a[1] + members - s // 2, members)

    attended = pl.pallas_call(
        attend_body,
        grid_spec=pltpu.PrefetchScalarGridSpec(
            num_scalar_prefetch=1,
            grid=(blocks,),
            in_specs=[whole(query.shape)] * members
            + [whole(near.shape)] * 2
            + [pl.BlockSpec((rank, LANES), lambda s, a: (0, 2 * group_at(s, a) + s % 2))] * 2,
            out_specs=[whole(part)] * members,
            scratch_shapes=[
                pltpu.VMEM((blocks + 1, rows, LANES), BF),
                pltpu.VMEM((2 * rows, 2 * LANES), BF),
                pltpu.VMEM((keys_here, rank), BF),
                pltpu.VMEM((keys_here, LANES), BF),
                pltpu.VMEM((keys_here, 2 * LANES), BF),
                pltpu.VMEM((2 * rows, keys_here), F32),
                pltpu.VMEM((2 * rows, LANES), F32),
                pltpu.VMEM((rows, LANES), F32),
            ],
        ),
        out_shape=[jax.ShapeDtypeStruct(part, BF)] * members,
        compiler_params=room(32),
        name="attend",
    )(at, query, *others, near, far, key_expand_weight, value_expand_weight)
    parts = [attended[0]] + [shifted(attended[k], "tp", k) for k in range(1, members)]
    half = model // 2
    mixed, own_a, own_b = pl.pallas_call(
        merge_body,
        grid_spec=pltpu.PrefetchScalarGridSpec(
            num_scalar_prefetch=1,
            grid=(1,),
            in_specs=[whole(part)] * members
            + [whole(out_weight.shape)] * members
            + [pl.BlockSpec((own, model), lambda s, a: (a[1], 0)), whole((1, model))],
            out_specs=[whole((own, model)), whole((own, half)), whole((own, half))],
        ),
        out_shape=[
            jax.ShapeDtypeStruct((own, model), F32),
            jax.ShapeDtypeStruct((own, half), BF),
            jax.ShapeDtypeStruct((own, half), BF),
        ],
        compiler_params=room(20),
        name="merge",
    )(at, *parts, *outs, residual, ffn_gain[None])
    below_a = shifted(own_a, "tp", 1)
    above_b = shifted(own_b, "tp", -1)
    below_b = shifted(own_b, "tp", 1)
    above_a = shifted(own_a, "tp", -1)
    across_a = shifted(below_a, "tp", 1)
    across_b = shifted(above_b, "tp", -1)

    phases = 4
    cut = model // phases
    weights = gathered.reshape(phases, sp_count // phases, 3, share, hidden_here)
    terms = pl.pallas_call(
        feed_body,
        in_specs=[pl.BlockSpec(memory_space=pltpu.VMEM)] * 8 + [pl.BlockSpec(memory_space=pl.ANY)],
        out_specs=[pl.BlockSpec(memory_space=pltpu.VMEM)] * 8,
        out_shape=[jax.ShapeDtypeStruct((own, half), BF)] * 8,
        scratch_shapes=[
            pltpu.VMEM((phases, rows, cut), BF),
            pltpu.VMEM(weights.shape, BF),
            pltpu.VMEM((rows, hidden_here), F32),
            pltpu.VMEM((rows, hidden_here), F32),
            pltpu.VMEM((rows, hidden_here), BF),
            pltpu.SemaphoreType.DMA((2, phases, sp_count // phases)),
        ],
        compiler_params=room(40),
        name="feed",
    )(own_a, own_b, below_a, below_b, across_a, across_b, above_a, above_b, weights)
    mine_a, down_a, far_a, up_a, mine_b, down_b, far_b, up_b = terms
    far_a = shifted(far_a, "tp", -1)
    far_b = shifted(far_b, "tp", 1)
    from_above_b = shifted(down_b, "tp", -1)
    from_below_a = shifted(up_a, "tp", 1)
    sum_b = (up_b.astype(F32) + far_b.astype(F32)).astype(BF)
    from_below_b = shifted(sum_b, "tp", 1)
    sum_a = (down_a.astype(F32) + far_a.astype(F32)).astype(BF)
    from_above_a = shifted(sum_a, "tp", -1)
    return pl.pallas_call(
        close_body,
        in_specs=[pl.BlockSpec(memory_space=pltpu.VMEM)] * 7,
        out_specs=pl.BlockSpec(memory_space=pltpu.VMEM),
        out_shape=jax.ShapeDtypeStruct((own, model), BF),
        compiler_params=room(8),
        name="close",
    )(mixed, mine_a, from_above_a, from_below_a, mine_b, from_above_b, from_below_b)


def solution(mesh):
    groups, sp_count, members = mesh.devices.shape
    finer = Mesh(
        mesh.devices.reshape(groups, sp_count // CORES, CORES, members),
        ("grp", "z", "core", "tp"),
    )
    tokens = ("grp", "z", "core")
    return jax.shard_map(
        layer,
        mesh=finer,
        in_specs=(
            P(tokens, "tp"),
            P(tokens, "tp"),
            P(tokens, None),
            P(tokens, None),
            P(),
            P(),
            P(),
            P(tokens, None),
            P("tp", None),
            P(),
            P(("z", "core"), "tp"),
            P(("z", "core"), "tp"),
            P("tp", ("z", "core")),
        ),
        out_specs=P(tokens + ("tp",), None),
        check_vma=False,
    )
```
